256 devices in a mesh: grp: 2 (over z), sp: 16 (over y, core), tp: 8 (over x).
Axes of the slice: x: 8, y: 8, z: 2, core: 2. Of those that a mesh axis runs over, the one named last changes fastest.
The devices are a block of a 8x8x16 slice.
Arguments:
- tokens_in: bfloat16 [8192, 2048], P(('grp', 'sp'), 'tp'), parts along dimension 0, may hold values from -8 to 8
- out_gate: bfloat16 [3, 2048, 2048], P(None, 'sp', 'tp'), may hold values from -0.125 to 0.125
- in_gate: bfloat16 [3, 2048, 2048], P(None, 'sp', 'tp'), may hold values from -0.125 to 0.125
- value_proj: bfloat16 [3, 2048, 2048], P(None, 'sp', 'tp'), may hold values from -0.125 to 0.125
- mix_proj: bfloat16 [3, 2048, 2048], P(None, 'sp', 'tp'), may hold values from -0.125 to 0.125
- conv_taps: float32 [3, 3, 2048], P(None, None, 'tp'), may hold values from -3.5 to 3.5
- norm_gains: float32 [3, 2048], P(None, 'tp'), may hold values from 0.1 to 1.9
- final_gain: float32 [2048], P('tp'), may hold values from 0.1 to 1.9
Outputs:
- normed_out: bfloat16 [8192, 2048], P(('grp', 'sp'), 'tp'), parts along dimension 0
The draws below stay inside these ranges and needn't reach their ends.
There are 2 independent parts, one for each index of `grp`. The reference program is written for one: setup_inputs(seed, part) draws one part's arguments, and reference() takes and returns one part's arrays. A program takes and returns all parts, laid end to end along the dimension named above; an argument that names none is the same for every part. Nothing has to cross between parts.
All inputs are finite; a program needn't handle non-finite values.
Results may differ from the reference program's by a relative error of at most 0.025.
Values may be sent and summed in bfloat16 or wider, within the bound.
No kernel may reach another device: no remote copies, remote signals or barrier semaphores. Data moves between devices by JAX's collectives and lax.ppermute only.
A program may use at most 64 MiB of HBM per device.

```python
import jax
import jax.numpy as jnp
from jax import lax

D = 2048
TAPS = 3
LAYERS = 3
TOKENS = 4096


def draw_tokens_in(key, part):
    keys = jax.random.split(jax.random.fold_in(key, 11), 2)
    ramp = jnp.exp(jnp.linspace(jnp.log(0.5), jnp.log(2.0), D)).astype(jnp.float32)
    rough = jnp.exp(jax.random.uniform(keys[1], (D,), jnp.float32, -0.35, 0.35))
    values = jax.random.normal(keys[0], (TOKENS, D), jnp.float32) * ramp * rough
    return jnp.clip(values, -8.0, 8.0).astype(jnp.bfloat16)


def block_levels(own_key, shape, shards, smallest, high):
    loudness, own = 1.0, jax.random.fold_in(own_key, 6)
    for axis_at, blocks in shards:
        heights = jnp.exp(jax.random.uniform(jax.random.fold_in(own, axis_at), (blocks,), jnp.float32, smallest / len(shards), high / len(shards)))
        loudness = loudness * jnp.repeat(heights, shape[axis_at] // blocks).reshape([-1 if axis == axis_at else 1 for axis in range(len(shape))])
    return loudness


def normal_values(rng, shape, width, most, cuts=(), held_as=jnp.bfloat16):
    entries = jax.random.normal(rng, shape, jnp.float32) * width
    if len(cuts) > 0:
        entries = block_levels(rng, shape, cuts, -0.22, 0.18) * entries
    return jnp.clip(entries, min=-most, max=most).astype(held_as)


def setup_inputs(seed: int = 0, part: int = 0) -> dict:
    arg_keys = jax.random.split(jax.random.key(seed), 9)
    own_keys = jax.random.split(jax.random.fold_in(arg_keys[8], part), 9)
    tokens_in = draw_tokens_in(jax.random.fold_in(jax.random.fold_in(arg_keys[8], part), 71), part)
    out_gate = normal_values(arg_keys[1], (LAYERS, D, D), D ** -0.5, 0.125, ((1, 16), (2, 8)))
    in_gate = normal_values(arg_keys[2], (LAYERS, D, D), D ** -0.5, 0.125, ((1, 16), (2, 8)))
    value_proj = normal_values(arg_keys[3], (LAYERS, D, D), D ** -0.5, 0.125, ((1, 16), (2, 8)))
    mix_proj = normal_values(arg_keys[4], (LAYERS, D, D), D ** -0.5, 0.125, ((1, 16), (2, 8)))
    conv_taps = normal_values(arg_keys[5], (LAYERS, TAPS, D), TAPS ** -0.5, 3.5, ((2, 8),), jnp.float32)
    norm_gains = jnp.clip(1.0 + 0.18 * jax.random.normal(arg_keys[6], (LAYERS, D), jnp.float32), 0.1, 1.9)
    final_gain = jnp.clip(1.0 + 0.18 * jax.random.normal(arg_keys[7], (D,), jnp.float32), 0.1, 1.9)
    return {"tokens_in": tokens_in, "out_gate": out_gate, "in_gate": in_gate, "value_proj": value_proj, "mix_proj": mix_proj, "conv_taps": conv_taps, "norm_gains": norm_gains, "final_gain": final_gain}


epsilon = 1e-06

def reference(tokens_in, out_gate, in_gate, value_proj, mix_proj, conv_taps, norm_gains, final_gain):
    stream = tokens_in.astype(jnp.float32)
    reach = TAPS - 1
    for layer_index in range(LAYERS):
        scale = lax.rsqrt(lax.optimization_barrier(jnp.sum(stream * stream, axis=1, keepdims=True)) / D + epsilon)
        normed = (stream * norm_gains[layer_index]).astype(jnp.bfloat16)
        out_gates = (jnp.dot(normed, out_gate[layer_index], preferred_element_type=jnp.float32) * scale).astype(jnp.bfloat16)
        in_gates = (jnp.dot(normed, in_gate[layer_index], preferred_element_type=jnp.float32) * scale).astype(jnp.bfloat16)
        values = (jnp.dot(normed, value_proj[layer_index], preferred_element_type=jnp.float32) * scale).astype(jnp.bfloat16)
        product_v = (in_gates.astype(jnp.float32) * values.astype(jnp.float32)).astype(jnp.bfloat16)
        padded = jnp.concatenate([jnp.zeros((reach, D), jnp.bfloat16), product_v], axis=0)
        convolved = jnp.zeros((TOKENS, D), jnp.float32)
        for tap_index in range(TAPS):
            convolved = convolved + padded[tap_index:tap_index + TOKENS].astype(jnp.float32) * conv_taps[layer_index, tap_index]
        gated = (out_gates.astype(jnp.float32) * convolved).astype(jnp.bfloat16)
        stream = stream + jnp.dot(gated, mix_proj[layer_index], preferred_element_type=jnp.float32)
    scale = lax.rsqrt(lax.optimization_barrier(jnp.sum(stream * stream, axis=1, keepdims=True)) / D + epsilon)
    return (stream * scale * final_gain).astype(jnp.bfloat16)
```

```python
import functools

import jax
import jax.numpy as jnp
from jax import lax
from jax.experimental import pallas as pl
from jax.experimental.pallas import tpu as pltpu
from jax.sharding import PartitionSpec as P

TAPS = 3
LAYERS = 3
HALO = 8

epsilon = 1e-06


OFFSETS = (0, -1, 1, -2, 2, -3, 3, 4)


def shifted(x, by):
    n = lax.axis_size("tp")
    return lax.ppermute(x, "tp", [(i, (i + by) % n) for i in range(n)])


def gather_blocks(x):
    half = x.shape[0] // 16 * 8
    from_m2, from_p2 = shifted(x, 2), shifted(x, -2)
    from_m1, from_p1 = shifted(x, 1), shifted(x, -1)
    from_m3, from_p3 = shifted(from_m2, 1), shifted(from_p2, -1)
    opposite = jnp.concatenate([shifted(from_m2[:half], 2), shifted(from_p2[half:], -2)], axis=0)
    return [x, from_m1, from_p1, from_m2, from_p2, from_m3, from_p3, opposite]


def block_of(j):
    n = lax.axis_size("tp")
    return lax.rem(lax.axis_index("tp") + (OFFSETS[j] + n), n)


def start_weights(w_hbm, first, count, w_ref, sem):
    depth = w_ref.shape[1] // len(OFFSETS)
    copies = []
    for j in range(len(OFFSETS)):
        rows = pl.ds(pl.multiple_of(block_of(j) * depth, depth), depth)
        copy = pltpu.make_async_copy(
            w_hbm.at[pl.ds(first, count), rows, :], w_ref.at[:, pl.ds(j * depth, depth), :], sem.at[j]
        )
        copy.start()
        copies.append(copy)
    return copies


def in_kernel(width, *refs):
    n = len(OFFSETS)
    blocks, (w_hbm, inv_gains, taps, gated, w_ref, a_ref, sem) = refs[:n], refs[n:]
    copies = start_weights(w_hbm, 0, 3, w_ref, sem)
    depth = blocks[0].shape[1]
    squares = None
    for j in range(n):
        block = blocks[j][...]
        a_ref[:, j * depth : (j + 1) * depth] = block
        entries = block.astype(jnp.float32) * inv_gains[pl.ds(block_of(j), 1), :]
        entries = entries * entries
        squares = entries if squares is None else squares + entries
    scale = lax.rsqrt(jnp.sum(squares, axis=1, keepdims=True) / width + epsilon)
    for copy in copies:
        copy.wait()
    a = a_ref[...]
    out_gates, in_gates, values = [
        (jnp.dot(a, w_ref[p], preferred_element_type=jnp.float32) * scale).astype(jnp.bfloat16).astype(jnp.float32)
        for p in range(3)
    ]
    product_v = (in_gates * values).astype(jnp.bfloat16).astype(jnp.float32)
    convolved = product_v * taps[TAPS - 1 : TAPS, :]
    for k in range(TAPS - 1):
        convolved = convolved + pltpu.roll(product_v, TAPS - 1 - k, 0) * taps[k : k + 1, :]
    gated[...] = (out_gates * convolved).astype(jnp.bfloat16)


def out_kernel(*refs):
    n = len(OFFSETS)
    blocks, (w_hbm, stream, gain, new_stream, normed, w_ref, a_ref, sem) = refs[:n], refs[n:]
    copies = start_weights(w_hbm, 3, 1, w_ref, sem)
    depth = blocks[0].shape[1]
    for j in range(n):
        a_ref[:, j * depth : (j + 1) * depth] = blocks[j][...]
    for copy in copies:
        copy.wait()
    mixed = jnp.dot(a_ref[...], w_ref[0], preferred_element_type=jnp.float32)
    total = stream[...] + mixed
    new_stream[...] = total
    normed[...] = (total * gain[...]).astype(jnp.bfloat16)


def vmem(count):
    return [pl.BlockSpec(memory_space=pltpu.VMEM)] * count


def scratch(parts, rows, depth, width):
    n = len(OFFSETS)
    return [
        pltpu.VMEM((parts, n * depth, width), jnp.bfloat16),
        pltpu.VMEM((rows, n * depth), jnp.bfloat16),
        pltpu.SemaphoreType.DMA((n,)),
    ]


def in_projections(blocks, weights, inv_gains, taps):
    rows, depth = blocks[0].shape
    n = len(blocks)
    return pl.pallas_call(
        functools.partial(in_kernel, n * depth),
        out_shape=jax.ShapeDtypeStruct((rows, taps.shape[1]), jnp.bfloat16),
        in_specs=vmem(n) + [pl.BlockSpec(memory_space=pl.ANY)] + vmem(2),
        out_specs=pl.BlockSpec(memory_space=pltpu.VMEM),
        scratch_shapes=scratch(3, rows, depth, taps.shape[1]),
        compiler_params=pltpu.CompilerParams(vmem_limit_bytes=24 << 20),
        cost_estimate=pl.CostEstimate(flops=2 * rows * n * depth * 768, bytes_accessed=4 << 20, transcendentals=0),
        name="in_projections",
    )(*blocks, weights, inv_gains, taps)


def out_projection(blocks, weights, stream, gain):
    rows, depth = blocks[0].shape
    n = len(blocks)
    return pl.pallas_call(
        out_kernel,
        out_shape=(
            jax.ShapeDtypeStruct(stream.shape, jnp.float32),
            jax.ShapeDtypeStruct(stream.shape, jnp.bfloat16),
        ),
        in_specs=vmem(n) + [pl.BlockSpec(memory_space=pl.ANY)] + vmem(2),
        out_specs=tuple(vmem(2)),
        scratch_shapes=scratch(1, rows, depth, stream.shape[1]),
        compiler_params=pltpu.CompilerParams(vmem_limit_bytes=24 << 20),
        cost_estimate=pl.CostEstimate(flops=2 * rows * n * depth * 256, bytes_accessed=2 << 20, transcendentals=0),
        name="out_projection",
    )(*blocks, weights, stream, gain)


def sum_over_tp(x):
    n = lax.axis_size("tp")
    step = 1
    while step < n:
        x = x + lax.ppermute(x, "tp", [(i, i ^ step) for i in range(n)])
        step *= 2
    return x


def shards(tokens_in, out_gate, in_gate, value_proj, mix_proj, conv_taps, norm_gains, final_gain):
    packed = [
        lax.all_gather(
            jnp.stack([w[layer] for w in (out_gate, in_gate, value_proj, mix_proj)]), "sp", axis=1, tiled=True
        )
        for layer in range(LAYERS)
    ]
    peers = lax.axis_size("sp")
    before = lax.ppermute(tokens_in[-HALO:], "sp", [(i, i + 1) for i in range(peers - 1)])
    stream = jnp.concatenate([before, tokens_in], axis=0).astype(jnp.float32)
    inv_gains = 1.0 / lax.all_gather(norm_gains, "tp", axis=1)
    normed = (stream * norm_gains[0]).astype(jnp.bfloat16)
    for layer in range(LAYERS):
        gated = in_projections(gather_blocks(normed), packed[layer], inv_gains[layer], conv_taps[layer])
        gain = norm_gains[(layer + 1) % LAYERS][None, :]
        stream, normed = out_projection(gather_blocks(gated), packed[layer], stream, gain)
    stream = stream[HALO:]
    width = lax.axis_size("tp") * stream.shape[1]
    squares = sum_over_tp(jnp.sum(stream * stream, axis=1))
    scale = lax.rsqrt(squares / width + epsilon)[:, None]
    return (stream * scale * final_gain).astype(jnp.bfloat16)


def solution(mesh):
    in_specs = (
        P(("grp", "sp"), "tp"),
        P(None, "sp", "tp"),
        P(None, "sp", "tp"),
        P(None, "sp", "tp"),
        P(None, "sp", "tp"),
        P(None, None, "tp"),
        P(None, "tp"),
        P("tp"),
    )
    out_specs = P(("grp", "sp"), "tp")
    return jax.shard_map(shards, mesh=mesh, in_specs=in_specs, out_specs=out_specs, check_vma=False)
```
